32 devices in a mesh: sp: 8 (over z, y), dp: 4 (over x, core).
Axes of the slice: x: 2, y: 2, z: 4, core: 2. Of those that a mesh axis runs over, the one named last changes fastest.
Arguments:
- tokens: bfloat16 [8, 512, 2048], P('dp', 'sp'), may hold values from -6 to 6
- norm_gain: float32 [2048], replicated, may hold values from 0.1 to 1.9
- w_query: bfloat16 [2048, 4096], P(None, 'dp'), may hold values from -1 to 1
- w_key: bfloat16 [2048, 1024], P(None, 'dp'), may hold values from -1 to 1
- w_value: bfloat16 [2048, 1024], P(None, 'dp'), may hold values from -0.125 to 0.125
- break_bias: float32 [32], P('dp'), may hold values from -12 to -3
- w_out: bfloat16 [4096, 2048], P('dp'), may hold values from -0.09375 to 0.09375
Outputs:
- mixed: bfloat16 [8, 512, 2048], P('dp', 'sp')
The draws below stay inside these ranges and needn't reach their ends.
All inputs are finite; a program needn't handle non-finite values.
Results may differ from the reference program's by a relative error of at most 0.015.
Values may be sent and summed in bfloat16 or wider, within the bound.
A program may use at most 64 MiB of HBM per device.

```python
import math
import jax
import jax.numpy as jnp
from jax import lax

D = 2048
HEAD_DIM = 128
HEADS = 32
KV_HEADS = 8
BATCH = 8
GROUPS = 4
LEN = 512


def drawn_weight(key, salt, head_count):
    base = jnp.clip(jax.random.normal(jax.random.fold_in(key, salt), (D, head_count * HEAD_DIM), jnp.float32), -6.0, 6.0)
    base = base * D ** (-0.5)
    return base.astype(jnp.bfloat16)


def draw_tokens(key, part):
    noise = jnp.clip(jax.random.normal(jax.random.fold_in(key, 3), (BATCH, LEN, D), jnp.float32), -6.0, 6.0)
    return noise.astype(jnp.bfloat16)


def draw_w_query(key, part):
    return drawn_weight(key, 5, HEADS)


def draw_w_key(key, part):
    return drawn_weight(key, 6, KV_HEADS)


def draw_break_bias(key, part):
    key_choose, key_slow, key_fast = jax.random.split(jax.random.fold_in(key, 7), 3)
    slow_shift = -math.log(LEN)
    slow_heads = jax.random.bernoulli(key_choose, 0.5, (HEADS,))
    slow_values = slow_shift + jax.random.uniform(key_slow, (HEADS,), jnp.float32, -2.0, 0.0)
    fast_values = jax.random.uniform(key_fast, (HEADS,), jnp.float32, -4.7, -3.5)
    return jnp.where(slow_heads, slow_values, fast_values)


def block_levels(rng, dims, cuts, low, top_value):
    loudness, own = 1.0, jax.random.fold_in(rng, 6)
    for position, shards_of in cuts:
        steps = jnp.exp(jax.random.uniform(jax.random.fold_in(own, position), (shards_of,), jnp.float32, low / len(cuts), top_value / len(cuts)))
        loudness = loudness * jnp.repeat(steps, dims[position] // shards_of).reshape([-1 if axis == position else 1 for axis in range(len(dims))])
    return loudness


def normal_values(key, dims, width, most, shards=(), kind=jnp.bfloat16):
    drawn = width * jax.random.normal(key, dims, jnp.float32)
    if shards:
        drawn = drawn * block_levels(key, dims, shards, -0.22, 0.18)
    return jnp.clip(drawn, -most, most).astype(kind)


def setup_inputs(seed: int = 0) -> dict:
    splits = jax.random.split(jax.random.key(seed), 8)
    tokens = draw_tokens(jax.random.fold_in(splits[7], 71), 0)
    norm_gain = jnp.clip(1.0 + 0.18 * jax.random.normal(splits[1], (D,), jnp.float32), 0.1, 1.9)
    w_query = draw_w_query(jax.random.fold_in(splits[7], 71), 0)
    w_key = draw_w_key(jax.random.fold_in(splits[7], 71), 0)
    w_value = normal_values(splits[4], (D, KV_HEADS * HEAD_DIM), D ** -0.5, 0.125, ((1, 4),))
    break_bias = draw_break_bias(jax.random.fold_in(splits[7], 71), 0)
    w_out = normal_values(splits[6], (HEADS * HEAD_DIM, D), (HEADS * HEAD_DIM) ** -0.5, 0.09375, ((0, 4),))
    return dict(tokens=tokens, norm_gain=norm_gain, w_query=w_query, w_key=w_key, w_value=w_value, break_bias=break_bias, w_out=w_out)


EPS = 1e-06

def normalize(tokens):
    widened = tokens.astype(jnp.float32)
    return widened * lax.rsqrt(lax.optimization_barrier(jnp.mean(widened * widened, axis=-1, keepdims=True)) + EPS)

def stick_item(operands):
    query_data, key_data, value_data, bias_term = operands
    seq_length = query_data.shape[0]
    block_size = math.gcd(seq_length, 512)
    head_scale = query_data.shape[1] ** (-0.5)
    key_pos = jnp.arange(seq_length, dtype=jnp.int32)

    def query_block(block_index):
        query_rows = lax.dynamic_slice_in_dim(query_data, block_index * block_size, block_size, 0)
        query_pos = block_index * block_size + jnp.arange(block_size, dtype=jnp.int32)
        scores = jnp.dot(query_rows, key_data.T, preferred_element_type=jnp.float32) * head_scale + bias_term
        causal = key_pos[None, :] < query_pos[:, None]
        log_keep = jnp.where(causal, jax.nn.log_sigmoid(-scores), 0.0)
        after_sum = lax.cumsum(log_keep, axis=1, reverse=True) - log_keep
        weights = jnp.where(causal, jnp.exp(jax.nn.log_sigmoid(scores) + after_sum), 0.0).astype(jnp.bfloat16)
        return jnp.dot(weights, value_data, preferred_element_type=jnp.float32).astype(jnp.bfloat16)
    blocks = lax.map(query_block, jnp.arange(seq_length // block_size, dtype=jnp.int32))
    return blocks.reshape(seq_length, query_data.shape[1])

def reference(tokens, norm_gain, w_query, w_key, w_value, break_bias, w_out):
    sequences, seq_length, model_width = tokens.shape
    head_ratio = HEADS // KV_HEADS
    normed = (normalize(tokens) * norm_gain).astype(jnp.bfloat16).reshape(sequences * seq_length, model_width)

    def heads_first(weight, head_count):
        projected = jnp.dot(normed, weight, preferred_element_type=jnp.float32).astype(jnp.bfloat16)
        return projected.reshape(sequences, seq_length, head_count, HEAD_DIM).transpose(0, 2, 1, 3)
    query_data = heads_first(w_query, HEADS).reshape(sequences * HEADS, seq_length, HEAD_DIM)
    key_data = jnp.repeat(heads_first(w_key, KV_HEADS), head_ratio, axis=1).reshape(sequences * HEADS, seq_length, HEAD_DIM)
    value_data = jnp.repeat(heads_first(w_value, KV_HEADS), head_ratio, axis=1).reshape(sequences * HEADS, seq_length, HEAD_DIM)
    bias_all = jnp.broadcast_to(break_bias[None, :], (sequences, HEADS)).reshape(sequences * HEADS)
    attended = lax.map(stick_item, (query_data, key_data, value_data, bias_all))
    group_heads = HEADS // GROUPS
    attended = attended.reshape(sequences, GROUPS, group_heads, seq_length, HEAD_DIM)
    out_groups = w_out.reshape(GROUPS, group_heads * HEAD_DIM, model_width)
    projected = jnp.zeros((sequences * seq_length, model_width), jnp.float32)
    for group_index in range(GROUPS):
        piece_rows = attended[:, group_index].transpose(0, 2, 1, 3).reshape(sequences * seq_length, group_heads * HEAD_DIM)
        partial_value = jnp.dot(piece_rows, out_groups[group_index], preferred_element_type=jnp.float32).astype(jnp.bfloat16)
        partial_value = lax.optimization_barrier(partial_value)
        projected = projected + partial_value.astype(jnp.float32)
    return normalize(projected).astype(jnp.bfloat16).reshape(sequences, seq_length, model_width)
```

```python
import functools
import math

import jax
import jax.numpy as jnp
from jax import lax
from jax.experimental import pallas as pl
from jax.experimental.pallas import tpu as pltpu
from jax.sharding import PartitionSpec as P

HEAD_DIM = 128


EPS = 1e-06


def normalize(tokens):
    widened = tokens.astype(jnp.float32)
    return widened * lax.rsqrt(jnp.mean(widened * widened, axis=-1, keepdims=True) + EPS)


def head_major(normed, weight, copies):
    model_width = weight.shape[0]
    head_count = weight.shape[1] // HEAD_DIM
    result = jnp.einsum(
        "ntd,dhc->nhtc",
        normed,
        weight.reshape(model_width, head_count, HEAD_DIM),
        preferred_element_type=jnp.float32,
    ).astype(jnp.bfloat16)
    return jnp.repeat(result, copies, axis=1)


def stick_item(operands):
    query_data, key_data, value_data, bias_term = operands
    seq_length = query_data.shape[0]
    block_size = math.gcd(seq_length, 512)
    head_scale = HEAD_DIM ** (-0.5)
    offsets = jnp.arange(block_size, dtype=jnp.int32)

    def query_block(block_index):
        query_rows = lax.dynamic_slice_in_dim(query_data, block_index * block_size, block_size, 0)
        query_pos = block_index * block_size + offsets

        def key_block(step_count, carry):
            carried, accumulated = carry
            key_index = block_index - step_count
            key_rows = lax.dynamic_slice_in_dim(key_data, key_index * block_size, block_size, 0)
            value_rows = lax.dynamic_slice_in_dim(value_data, key_index * block_size, block_size, 0)
            key_pos = key_index * block_size + offsets
            scores = (
                jnp.einsum("qc,kc->qk", query_rows, key_rows, preferred_element_type=jnp.float32)
                * head_scale
                + bias_term
            )
            causal = key_pos[None, :] < query_pos[:, None]
            log_keep = jnp.where(causal, jax.nn.log_sigmoid(-scores), 0.0)
            after_sum = lax.cumsum(log_keep, axis=1, reverse=True) - log_keep + carried[:, None]
            weights = jnp.where(
                causal, jnp.exp(jax.nn.log_sigmoid(scores) + after_sum), 0.0
            ).astype(jnp.bfloat16)
            accumulated = accumulated + jnp.dot(
                weights, value_rows, preferred_element_type=jnp.float32
            )
            return (carried + jnp.sum(log_keep, axis=1), accumulated)

        initial = (
            jnp.zeros((block_size,), jnp.float32),
            jnp.zeros((block_size, HEAD_DIM), jnp.float32),
        )
        carried, accumulated = lax.fori_loop(0, block_index + 1, key_block, initial)
        return accumulated.astype(jnp.bfloat16)

    blocks = lax.map(query_block, jnp.arange(seq_length // block_size, dtype=jnp.int32))
    return blocks.reshape(seq_length, HEAD_DIM)


def exchanged(tokens, norm_gain, w_query, w_key, w_value, break_bias, w_out):
    own_seqs = tokens.shape[0]
    seq_count = lax.axis_size("dp") * own_seqs
    seq_parts = lax.axis_size("sp")
    local_heads = w_query.shape[1] // HEAD_DIM
    copies = local_heads // (w_key.shape[1] // HEAD_DIM)
    tok_rows = tokens.shape[1]
    model_width = tokens.shape[2]
    item_count = seq_count * local_heads
    normed = (normalize(lax.all_gather(tokens, "dp", axis=0, tiled=True)) * norm_gain).astype(
        jnp.bfloat16
    )
    combined = jnp.concatenate(
        (
            head_major(normed, w_query, 1),
            head_major(normed, w_key, copies),
            head_major(normed, w_value, copies),
        ),
        axis=3,
    )
    arrived = lax.all_to_all(
        combined.reshape(item_count, tok_rows, 3 * HEAD_DIM),
        "sp",
        split_axis=0,
        concat_axis=1,
        tiled=True,
    )
    query_data = arrived[:, :, :HEAD_DIM]
    key_data = arrived[:, :, HEAD_DIM : 2 * HEAD_DIM]
    value_data = arrived[:, :, 2 * HEAD_DIM :]
    per_device = item_count // seq_parts
    item_ids = lax.axis_index("sp") * per_device + jnp.arange(per_device, dtype=jnp.int32)
    local_ids = item_ids % local_heads
    bias_items = jnp.sum(
        jnp.where(
            local_ids[:, None] == jnp.arange(local_heads, dtype=jnp.int32)[None, :],
            break_bias[None, :],
            0.0,
        ),
        axis=1,
    )
    attended = lax.map(stick_item, (query_data, key_data, value_data, bias_items))
    returned = lax.all_to_all(attended, "sp", split_axis=1, concat_axis=0, tiled=True)
    grouped = returned.reshape(seq_count, local_heads, tok_rows, HEAD_DIM)
    out_weight = w_out.reshape(local_heads, HEAD_DIM, model_width)
    term_rows = jnp.einsum(
        "nhtc,hcd->ntd", grouped, out_weight, preferred_element_type=jnp.float32
    ).astype(jnp.bfloat16)
    term_rows = lax.optimization_barrier(term_rows)
    summed = lax.psum_scatter(
        term_rows.astype(jnp.float32).astype(jnp.bfloat16), "dp", scatter_dimension=0, tiled=True
    ).astype(jnp.float32)
    return normalize(summed).astype(jnp.bfloat16)


def remote(src, dst, send_sem, recv_sem, sp, dp):
    return pltpu.make_async_remote_copy(
        src_ref=src,
        dst_ref=dst,
        send_sem=send_sem,
        recv_sem=recv_sem,
        device_id={"sp": sp, "dp": dp},
        device_id_type=pl.DeviceIdType.MESH,
    )


def greet(sp, dp):
    pl.semaphore_signal(
        pltpu.get_barrier_semaphore(),
        inc=1,
        device_id={"sp": sp, "dp": dp},
        device_id_type=pl.DeviceIdType.MESH,
    )


def loop(count, body):
    lax.fori_loop(0, count, lambda step, carry: (body(step), carry)[1], 0)


def gather_kernel(sp_count, dp_count, x_ref, out_ref, send_a, recv_a, send_x, recv_x, send_p, recv_p):
    my_sp, my_dp = lax.axis_index("sp"), lax.axis_index("dp")
    own, _, part, _ = x_ref.shape
    pairs = dp_count // 2
    my_x, my_core = my_dp // 2, lax.rem(my_dp, 2)
    other = my_x * 2 + 1 - my_core
    at_home = my_sp // own == my_dp

    def greet_source(step):
        @pl.when(jnp.logical_not(jnp.logical_and(at_home, step == my_sp)))
        def _():
            greet(step, my_sp // own)

    loop(sp_count, greet_source)
    for step in range(1, dp_count):
        greet(my_sp, lax.rem(my_dp + step, dp_count))
    pl.semaphore_wait(
        pltpu.get_barrier_semaphore(), sp_count + dp_count - 1 - at_home.astype(jnp.int32)
    )

    def first_copy(s, q):
        return remote(
            x_ref.at[s, q], out_ref.at[my_sp, q], send_a.at[s, q], recv_a.at[my_sp], my_dp * own + s, q
        )

    def is_self(s, q):
        return jnp.logical_and(my_dp * own + s == my_sp, q == my_dp)

    for s in range(own):
        for q in range(dp_count):

            @pl.when(jnp.logical_not(is_self(s, q)))
            def _():
                first_copy(s, q).start()

            @pl.when(is_self(s, q))
            def _():
                pltpu.make_async_copy(
                    x_ref.at[s, q], out_ref.at[my_sp, q], recv_a.at[my_sp]
                ).start()

    def across(j, step):
        block = out_ref.at[j, my_dp]
        target = lax.rem(my_x + step, pairs) * 2 + my_core
        return remote(block, block, send_x.at[step - 1, j], recv_x.at[step - 1, j], my_sp, target)

    def inside(j, x):
        block = out_ref.at[j, x * 2 + my_core]
        return remote(block, block, send_p.at[x, j], recv_p.at[x, j], my_sp, other)

    def arrived(j, q, sem):
        block = out_ref.at[j, q]
        pltpu.make_async_copy(block, block, sem).wait()

    def hand_on(step):
        j = lax.rem(my_sp + step, sp_count)
        arrived(j, my_dp, recv_a.at[j])
        for hop in range(1, pairs):
            across(j, hop).start()
        inside(j, my_x).start()

    loop(sp_count, hand_on)

    def relay(step):
        j = lax.rem(my_sp + step, sp_count)
        for hop in range(1, pairs):
            x = lax.rem(my_x - hop + pairs, pairs)
            arrived(j, x * 2 + my_core, recv_x.at[hop - 1, j])
            inside(j, x).start()

    loop(sp_count, relay)

    def finish(j):
        for x in range(pairs):
            arrived(j, x * 2 + 1 - my_core, recv_p.at[x, j])
            inside(j, x).wait_send()
        for hop in range(1, pairs):
            across(j, hop).wait_send()

    loop(sp_count, finish)
    for s in range(own):
        for q in range(dp_count):

            @pl.when(jnp.logical_not(is_self(s, q)))
            def _():
                first_copy(s, q).wait_send()


def gather_sequence(blocks, sp_count):
    own, dp_count, part, width = blocks.shape
    pairs = dp_count // 2
    return pl.pallas_call(
        functools.partial(gather_kernel, sp_count, dp_count),
        out_shape=jax.ShapeDtypeStruct((sp_count, dp_count, part, width), blocks.dtype),
        in_specs=[pl.BlockSpec(memory_space=pltpu.VMEM)],
        out_specs=pl.BlockSpec(memory_space=pltpu.VMEM),
        scratch_shapes=[
            pltpu.SemaphoreType.DMA((own, dp_count)),
            pltpu.SemaphoreType.DMA((sp_count,)),
            pltpu.SemaphoreType.DMA((pairs - 1, sp_count)),
            pltpu.SemaphoreType.DMA((pairs - 1, sp_count)),
            pltpu.SemaphoreType.DMA((pairs, sp_count)),
            pltpu.SemaphoreType.DMA((pairs, sp_count)),
        ],
        compiler_params=pltpu.CompilerParams(collective_id=1, has_side_effects=True),
        name="gather_sequence",
    )(blocks)


def attention_kernel(block, bias_ref, q_ref, k_ref, v_ref, o_ref):
    length = q_ref.shape[0]
    log2e = math.log2(math.e)
    bias = bias_ref[pl.program_id(0)] * log2e
    scale = HEAD_DIM ** (-0.5) * log2e
    row = lax.broadcasted_iota(jnp.int32, (2 * block, 2 * block), 0)
    col = lax.broadcasted_iota(jnp.int32, (2 * block, 2 * block), 1)
    row = jnp.where(row >= block, row - block, row)
    summing = jnp.where(jnp.logical_or(col >= block, row > col), 1.0, 0.0).astype(jnp.bfloat16)
    at_row = lax.broadcasted_iota(jnp.int32, (block, block), 0)
    at_col = lax.broadcasted_iota(jnp.int32, (block, block), 1)
    causal = at_col < at_row
    for r in range(length // block):
        rows = pl.ds(r * block, block)
        query = q_ref[rows, :]
        carried = None
        total = None
        for c in range(r, -1, -1):
            keys = pl.ds(c * block, block)
            scores = (
                lax.dot_general(
                    query,
                    k_ref[keys, :],
                    (((1,), (1,)), ((), ())),
                    preferred_element_type=jnp.float32,
                )
                * scale
                + bias
            )
            soft = jnp.log2(1.0 + jnp.exp2(-jnp.abs(scores)))
            log_keep = -jnp.maximum(scores, 0.0) - soft
            log_break = jnp.minimum(scores, 0.0) - soft
            if c == r:
                log_keep = jnp.where(causal, log_keep, 0.0)
            high = log_keep.astype(jnp.bfloat16)
            low = (log_keep - high.astype(jnp.float32)).astype(jnp.bfloat16)
            sums = jnp.dot(
                jnp.concatenate((high, low), axis=1), summing, preferred_element_type=jnp.float32
            )
            exponent = log_break + sums[:, :block]
            if carried is not None:
                exponent = exponent + carried
            weights = jnp.exp2(exponent)
            if c == r:
                weights = jnp.where(causal, weights, 0.0)
            term = jnp.dot(
                weights.astype(jnp.bfloat16), v_ref[keys, :], preferred_element_type=jnp.float32
            )
            carried = sums[:, block:] if carried is None else carried + sums[:, block:]
            total = term if total is None else total + term
        o_ref[rows, :] = total.astype(jnp.bfloat16)


def attention(query, keys, values, bias, copies):
    length, columns = query.shape
    heads = columns // HEAD_DIM
    block = math.gcd(length, 128)
    return pl.pallas_call(
        functools.partial(attention_kernel, block),
        grid=(heads,),
        out_shape=jax.ShapeDtypeStruct((length, columns), jnp.bfloat16),
        in_specs=[
            pl.BlockSpec(memory_space=pltpu.SMEM),
            pl.BlockSpec((length, HEAD_DIM), lambda h: (0, h)),
            pl.BlockSpec((length, HEAD_DIM), lambda h: (0, h // copies)),
            pl.BlockSpec((length, HEAD_DIM), lambda h: (0, h // copies)),
        ],
        out_specs=pl.BlockSpec((length, HEAD_DIM), lambda h: (0, h)),
        name="attention",
    )(bias, query, keys, values)


def return_kernel(
    sp_count, dp_count, own, p_ref, out_ref, from_core, summed, from_x, done,
    send_p, recv_p, send_x, recv_x, send_h, recv_h,
):
    my_sp, my_dp = lax.axis_index("sp"), lax.axis_index("dp")
    pairs = dp_count // 2
    my_x, my_core = my_dp // 2, lax.rem(my_dp, 2)
    other = my_x * 2 + 1 - my_core
    home_dp = my_sp // own
    at_home = home_dp == my_dp

    def greet_source(step):
        s, q = step // dp_count, lax.rem(step, dp_count)

        @pl.when(jnp.logical_not(jnp.logical_and(my_dp * own + s == my_sp, q == my_dp)))
        def _():
            greet(my_dp * own + s, q)

    loop(own * dp_count, greet_source)
    for step in range(1, dp_count):
        greet(my_sp, lax.rem(my_dp + step, dp_count))
    pl.semaphore_wait(
        pltpu.get_barrier_semaphore(), sp_count + dp_count - 1 - at_home.astype(jnp.int32)
    )

    def inside(j, hop):
        x = lax.rem(my_x + hop, pairs)
        return remote(
            p_ref.at[j, x * 2 + 1 - my_core],
            from_core.at[hop, j],
            send_p.at[hop, j],
            recv_p.at[hop, j],
            my_sp,
            other,
        )

    def across(j, hop):
        x = lax.rem(my_x + hop, pairs)
        return remote(
            summed.at[hop - 1, j],
            from_x.at[hop - 1, j],
            send_x.at[hop - 1, j],
            recv_x.at[hop - 1, j],
            my_sp,
            x * 2 + my_core,
        )

    def homeward(j):
        return remote(
            done.at[j],
            out_ref.at[lax.rem(my_sp, own), my_dp],
            send_h.at[j],
            recv_h.at[lax.rem(my_sp, own), my_dp],
            j,
            home_dp,
        )

    hops = list(range(1, pairs)) + [0]
    for hop in hops:
        loop(sp_count, lambda j: inside(j, hop).start())

    def send_sums(step):
        j = lax.rem(my_sp + step, sp_count)
        for hop in range(1, pairs):
            inside(j, hop).wait_recv()
            mine = p_ref[j, lax.rem(my_x + hop, pairs) * 2 + my_core].astype(jnp.float32)
            summed[hop - 1, j] = (mine + from_core[hop, j].astype(jnp.float32)).astype(jnp.bfloat16)
            across(j, hop).start()

    loop(sp_count, send_sums)

    def is_self(j):
        return jnp.logical_and(at_home, j == my_sp)

    def complete(step):
        j = lax.rem(my_sp + step, sp_count)
        inside(j, 0).wait_recv()
        total = p_ref[j, my_dp].astype(jnp.float32) + from_core[0, j].astype(jnp.float32)
        for hop in range(1, pairs):
            across(j, hop).wait_recv()
            total = total + from_x[hop - 1, j].astype(jnp.float32)
        done[j] = normalize(total).astype(jnp.bfloat16)

        @pl.when(jnp.logical_not(is_self(j)))
        def _():
            homeward(j).start()

        @pl.when(is_self(j))
        def _():
            pltpu.make_async_copy(
                done.at[j],
                out_ref.at[lax.rem(my_sp, own), my_dp],
                recv_h.at[lax.rem(my_sp, own), my_dp],
            ).start()

    loop(sp_count, complete)

    def finish(j):
        for hop in range(pairs):
            inside(j, hop).wait_send()
        for hop in range(1, pairs):
            across(j, hop).wait_send()

        @pl.when(jnp.logical_not(is_self(j)))
        def _():
            homeward(j).wait_send()

    loop(sp_count, finish)
    for s in range(own):
        for q in range(dp_count):
            block = out_ref.at[s, q]
            pltpu.make_async_copy(block, block, recv_h.at[s, q]).wait()


def return_home(partial, own):
    sp_count, dp_count, part, width = partial.shape
    pairs = dp_count // 2
    rows = (sp_count, part, width)
    return pl.pallas_call(
        functools.partial(return_kernel, sp_count, dp_count, own),
        out_shape=jax.ShapeDtypeStruct((own, dp_count, part, width), jnp.bfloat16),
        in_specs=[pl.BlockSpec(memory_space=pltpu.VMEM)],
        out_specs=pl.BlockSpec(memory_space=pltpu.VMEM),
        scratch_shapes=[
            pltpu.VMEM((pairs, *rows), jnp.bfloat16),
            pltpu.VMEM((pairs - 1, *rows), jnp.bfloat16),
            pltpu.VMEM((pairs - 1, *rows), jnp.bfloat16),
            pltpu.VMEM(rows, jnp.bfloat16),
            pltpu.SemaphoreType.DMA((pairs, sp_count)),
            pltpu.SemaphoreType.DMA((pairs, sp_count)),
            pltpu.SemaphoreType.DMA((pairs - 1, sp_count)),
            pltpu.SemaphoreType.DMA((pairs - 1, sp_count)),
            pltpu.SemaphoreType.DMA((sp_count,)),
            pltpu.SemaphoreType.DMA((own, dp_count)),
        ],
        compiler_params=pltpu.CompilerParams(collective_id=2, has_side_effects=True),
        name="return_home",
    )(partial)


def gathered(tokens, norm_gain, w_query, w_key, w_value, break_bias, w_out):
    own, tok_rows, width = tokens.shape
    sp_count, dp_count = lax.axis_size("sp"), lax.axis_size("dp")
    normed = (normalize(tokens) * norm_gain).astype(jnp.bfloat16)
    rows = gather_sequence(
        normed.reshape(own, dp_count, tok_rows // dp_count, width), sp_count
    ).reshape(sp_count * tok_rows, width)

    def project(weight):
        return jnp.dot(rows, weight, preferred_element_type=jnp.float32).astype(jnp.bfloat16)

    attended = attention(
        project(w_query),
        project(w_key),
        project(w_value),
        break_bias,
        w_query.shape[1] // w_key.shape[1],
    )
    partial = jnp.dot(attended, w_out, preferred_element_type=jnp.float32).astype(jnp.bfloat16)
    mixed = return_home(
        partial.reshape(sp_count, dp_count, tok_rows // dp_count, width), own
    )
    return mixed.reshape(own, tok_rows, width)


def local(tokens, *rest):
    sp_count, dp_count = lax.axis_size("sp"), lax.axis_size("dp")
    one_each = dp_count * tokens.shape[0] == sp_count
    if one_each and dp_count % 2 == 0 and dp_count > 2 and tokens.shape[1] % (16 * dp_count) == 0:
        return gathered(tokens, *rest)
    return exchanged(tokens, *rest)


def solution(mesh):
    return jax.shard_map(
        local,
        mesh=mesh,
        in_specs=(
            P("dp", "sp", None),
            P(),
            P(None, "dp"),
            P(None, "dp"),
            P(None, "dp"),
            P("dp"),
            P("dp", None),
        ),
        out_specs=P("dp", "sp", None),
        check_vma=False,
    )
```

```python
import functools
import math

import jax
import jax.numpy as jnp
from jax import lax
from jax.experimental import pallas as pl
from jax.experimental.pallas import tpu as pltpu
from jax.sharding import PartitionSpec as P

HEAD_DIM = 128


EPS = 1e-06


def normalize(tokens):
    widened = tokens.astype(jnp.float32)
    return widened * lax.rsqrt(jnp.mean(widened * widened, axis=-1, keepdims=True) + EPS)


def head_major(normed, weight, copies):
    model_width = weight.shape[0]
    head_count = weight.shape[1] // HEAD_DIM
    result = jnp.einsum(
        "ntd,dhc->nhtc",
        normed,
        weight.reshape(model_width, head_count, HEAD_DIM),
        preferred_element_type=jnp.float32,
    ).astype(jnp.bfloat16)
    return jnp.repeat(result, copies, axis=1)


def stick_item(operands):
    query_data, key_data, value_data, bias_term = operands
    seq_length = query_data.shape[0]
    block_size = math.gcd(seq_length, 512)
    head_scale = HEAD_DIM ** (-0.5)
    offsets = jnp.arange(block_size, dtype=jnp.int32)

    def query_block(block_index):
        query_rows = lax.dynamic_slice_in_dim(query_data, block_index * block_size, block_size, 0)
        query_pos = block_index * block_size + offsets

        def key_block(step_count, carry):
            carried, accumulated = carry
            key_index = block_index - step_count
            key_rows = lax.dynamic_slice_in_dim(key_data, key_index * block_size, block_size, 0)
            value_rows = lax.dynamic_slice_in_dim(value_data, key_index * block_size, block_size, 0)
            key_pos = key_index * block_size + offsets
            scores = (
                jnp.einsum("qc,kc->qk", query_rows, key_rows, preferred_element_type=jnp.float32)
                * head_scale
                + bias_term
            )
            causal = key_pos[None, :] < query_pos[:, None]
            log_keep = jnp.where(causal, jax.nn.log_sigmoid(-scores), 0.0)
            after_sum = lax.cumsum(log_keep, axis=1, reverse=True) - log_keep + carried[:, None]
            weights = jnp.where(
                causal, jnp.exp(jax.nn.log_sigmoid(scores) + after_sum), 0.0
            ).astype(jnp.bfloat16)
            accumulated = accumulated + jnp.dot(
                weights, value_rows, preferred_element_type=jnp.float32
            )
            return (carried + jnp.sum(log_keep, axis=1), accumulated)

        initial = (
            jnp.zeros((block_size,), jnp.float32),
            jnp.zeros((block_size, HEAD_DIM), jnp.float32),
        )
        carried, accumulated = lax.fori_loop(0, block_index + 1, key_block, initial)
        return accumulated.astype(jnp.bfloat16)

    blocks = lax.map(query_block, jnp.arange(seq_length // block_size, dtype=jnp.int32))
    return blocks.reshape(seq_length, HEAD_DIM)


def exchanged(tokens, norm_gain, w_query, w_key, w_value, break_bias, w_out):
    own_seqs = tokens.shape[0]
    seq_count = lax.axis_size("dp") * own_seqs
    seq_parts = lax.axis_size("sp")
    local_heads = w_query.shape[1] // HEAD_DIM
    copies = local_heads // (w_key.shape[1] // HEAD_DIM)
    tok_rows = tokens.shape[1]
    model_width = tokens.shape[2]
    item_count = seq_count * local_heads
    normed = (normalize(lax.all_gather(tokens, "dp", axis=0, tiled=True)) * norm_gain).astype(
        jnp.bfloat16
    )
    combined = jnp.concatenate(
        (
            head_major(normed, w_query, 1),
            head_major(normed, w_key, copies),
            head_major(normed, w_value, copies),
        ),
        axis=3,
    )
    arrived = lax.all_to_all(
        combined.reshape(item_count, tok_rows, 3 * HEAD_DIM),
        "sp",
        split_axis=0,
        concat_axis=1,
        tiled=True,
    )
    query_data = arrived[:, :, :HEAD_DIM]
    key_data = arrived[:, :, HEAD_DIM : 2 * HEAD_DIM]
    value_data = arrived[:, :, 2 * HEAD_DIM :]
    per_device = item_count // seq_parts
    item_ids = lax.axis_index("sp") * per_device + jnp.arange(per_device, dtype=jnp.int32)
    local_ids = item_ids % local_heads
    bias_items = jnp.sum(
        jnp.where(
            local_ids[:, None] == jnp.arange(local_heads, dtype=jnp.int32)[None, :],
            break_bias[None, :],
            0.0,
        ),
        axis=1,
    )
    attended = lax.map(stick_item, (query_data, key_data, value_data, bias_items))
    returned = lax.all_to_all(attended, "sp", split_axis=1, concat_axis=0, tiled=True)
    grouped = returned.reshape(seq_count, local_heads, tok_rows, HEAD_DIM)
    out_weight = w_out.reshape(local_heads, HEAD_DIM, model_width)
    term_rows = jnp.einsum(
        "nhtc,hcd->ntd", grouped, out_weight, preferred_element_type=jnp.float32
    ).astype(jnp.bfloat16)
    term_rows = lax.optimization_barrier(term_rows)
    summed = lax.psum_scatter(
        term_rows.astype(jnp.float32).astype(jnp.bfloat16), "dp", scatter_dimension=0, tiled=True
    ).astype(jnp.float32)
    return normalize(summed).astype(jnp.bfloat16)


def remote(src, dst, send_sem, recv_sem, sp, dp):
    return pltpu.make_async_remote_copy(
        src_ref=src,
        dst_ref=dst,
        send_sem=send_sem,
        recv_sem=recv_sem,
        device_id={"sp": sp, "dp": dp},
        device_id_type=pl.DeviceIdType.MESH,
    )


def greet(sp, dp):
    pl.semaphore_signal(
        pltpu.get_barrier_semaphore(),
        inc=1,
        device_id={"sp": sp, "dp": dp},
        device_id_type=pl.DeviceIdType.MESH,
    )


def loop(count, body):
    lax.fori_loop(0, count, lambda step, carry: (body(step), carry)[1], 0)


def layer_kernel(
    sp_count, dp_count, copies, block, x_ref, gain_ref, bias_ref, wq_hbm, wk_hbm, wv_hbm, wo_hbm, out_ref,
    wq, wk, wv, wo, normed, staged, rows_ref, q_ref, k_ref, v_ref, att_ref, p_ref, from_core, summed,
    from_x, done, home, load_sem, send_1, recv_1, send_2, recv_2, send_x, recv_x, send_p, recv_p,
    send_c, recv_c, send_s, recv_s, send_3, recv_3, send_4, recv_4,
):
    my_sp, my_dp = lax.axis_index("sp"), lax.axis_index("dp")
    own, _, part, width = x_ref.shape
    pairs = dp_count // 2
    my_x, my_core = my_dp // 2, lax.rem(my_dp, 2)
    other = my_x * 2 + 1 - my_core
    length = sp_count * dp_count * part

    def at_hop(hop):
        return lax.rem(my_x + hop, pairs)

    def peer(step):
        hop, flip = step // 2, step % 2
        return at_hop(hop) * 2 + (1 - my_core if flip else my_core)

    loop(sp_count - 1, lambda step: greet(lax.rem(my_sp + step + 1, sp_count), my_dp))
    for step in range(1, dp_count):
        greet(my_sp, lax.rem(my_dp + step, dp_count))

    loads = [
        pltpu.make_async_copy(source, target, load_sem.at[place])
        for place, (source, target) in enumerate(
            ((wq_hbm, wq), (wk_hbm, wk), (wv_hbm, wv), (wo_hbm, wo))
        )
    ]
    for load in loads:
        load.start()

    for s in range(own):
        for q in range(dp_count):
            normed[q, s] = (normalize(x_ref[s, q]) * gain_ref[...]).astype(jnp.bfloat16)
    staged[my_dp] = normed[my_dp]
    pl.semaphore_wait(pltpu.get_barrier_semaphore(), sp_count + dp_count - 2)

    def over_dp(step):
        q = peer(step)
        return remote(
            normed.at[q], staged.at[my_dp], send_1.at[step], recv_1.at[my_dp], my_sp, q
        )

    def arrived(ref, sem):
        pltpu.make_async_copy(ref, ref, sem).wait()

    order = list(range(2, dp_count)) + [1]
    for step in order:
        over_dp(step).start()

    def over_sp(e, s):
        i = e * own + s
        return remote(
            staged.at[e, s], rows_ref.at[my_sp, my_dp], send_2.at[i], recv_2.at[my_sp], i, my_dp
        )

    for step in [0, 1] + list(range(2, dp_count)):
        e = peer(step)
        if step:
            arrived(staged.at[e], recv_1.at[e])
        for s in range(own):

            @pl.when(e * own + s != my_sp)
            def _():
                over_sp(e, s).start()

            @pl.when(e * own + s == my_sp)
            def _():
                pltpu.make_async_copy(
                    staged.at[e, s], rows_ref.at[my_sp, my_dp], recv_2.at[my_sp]
                ).start()

    def across(j, hop):
        piece = rows_ref.at[j, my_dp]
        return remote(
            piece, piece, send_x.at[hop - 1, j], recv_x.at[hop - 1, j], my_sp, at_hop(hop) * 2 + my_core
        )

    def inside(j, x):
        piece = rows_ref.at[j, x * 2 + my_core]
        return remote(piece, piece, send_p.at[x, j], recv_p.at[x, j], my_sp, other)

    def hand_on(step):
        j = lax.rem(my_sp + step, sp_count)
        arrived(rows_ref.at[j, my_dp], recv_2.at[j])
        for hop in range(1, pairs):
            across(j, hop).start()
        inside(j, my_x).start()

    loop(sp_count, hand_on)

    def relay(step):
        j = lax.rem(my_sp + step, sp_count)
        for hop in range(1, pairs):
            x = at_hop(pairs - hop)
            arrived(rows_ref.at[j, x * 2 + my_core], recv_x.at[hop - 1, j])
            inside(j, x).start()

    loop(sp_count, relay)

    def finish_rows(j):
        for x in range(pairs):
            arrived(rows_ref.at[j, x * 2 + 1 - my_core], recv_p.at[x, j])

    loop(sp_count, finish_rows)
    for load in loads:
        load.wait()

    rows = rows_ref[...].reshape(length, width)

    def project(weight, target):
        columns = math.gcd(weight.shape[1], 256)

        def tile(n):
            at = pl.ds(pl.multiple_of(n * columns, columns), columns)
            target[:, at] = jnp.dot(
                rows, weight[:, at], preferred_element_type=jnp.float32
            ).astype(jnp.bfloat16)

        loop(weight.shape[1] // columns, tile)

    project(wk, k_ref)
    project(wv, v_ref)
    project(wq, q_ref)

    def head(h):
        mine = pl.ds(pl.multiple_of(h * HEAD_DIM, HEAD_DIM), HEAD_DIM)
        shared = pl.ds(pl.multiple_of(h // copies * HEAD_DIM, HEAD_DIM), HEAD_DIM)
        attend(block, bias_ref[h], q_ref[:, mine], k_ref[:, shared], v_ref[:, shared], att_ref, mine)

    loop(q_ref.shape[1] // HEAD_DIM, head)

    def chip_copy(j, hop):
        return remote(
            p_ref.at[j, at_hop(hop) * 2 + 1 - my_core],
            from_core.at[hop, j],
            send_c.at[hop, j],
            recv_c.at[hop, j],
            my_sp,
            other,
        )

    def sum_copy(j, hop):
        return remote(
            summed.at[hop - 1, j],
            from_x.at[hop - 1, j],
            send_s.at[hop - 1, j],
            recv_s.at[hop - 1, j],
            my_sp,
            at_hop(hop) * 2 + my_core,
        )

    hops = list(range(1, pairs)) + [0]
    some = math.gcd(sp_count, 2)
    group = sp_count // some
    wide = math.gcd(width, 512)
    tall = group * dp_count * part

    def send_sums(j):
        for hop in range(1, pairs):
            chip_copy(j, hop).wait_recv()
            mine = p_ref[j, at_hop(hop) * 2 + my_core].astype(jnp.float32)
            summed[hop - 1, j] = (mine + from_core[hop, j].astype(jnp.float32)).astype(jnp.bfloat16)
            sum_copy(j, hop).start()

    for r in range(some):
        heads = att_ref[r * tall : (r + 1) * tall, :]

        def out_tile(n):
            at = pl.ds(pl.multiple_of(n * wide, wide), wide)
            value = jnp.dot(heads, wo[:, at], preferred_element_type=jnp.float32)
            p_ref[r * group : (r + 1) * group, :, :, at] = value.astype(jnp.bfloat16).reshape(
                group, dp_count, part, wide
            )

        loop(width // wide, out_tile)
        for hop in hops:
            loop(group, lambda j: chip_copy(r * group + j, hop).start())
        loop(group, lambda j: send_sums(r * group + j))

    def to_sp(j):
        return remote(done.at[j], home.at[my_sp], send_3.at[j], recv_3.at[my_sp], j, my_dp)

    def complete(j):
        chip_copy(j, 0).wait_recv()
        total = p_ref[j, my_dp].astype(jnp.float32) + from_core[0, j].astype(jnp.float32)
        for hop in range(1, pairs):
            sum_copy(j, hop).wait_recv()
            total = total + from_x[hop - 1, j].astype(jnp.float32)
        done[j] = normalize(total).astype(jnp.bfloat16)

        @pl.when(j != my_sp)
        def _():
            to_sp(j).start()

        @pl.when(j == my_sp)
        def _():
            pltpu.make_async_copy(done.at[j], home.at[my_sp], recv_3.at[my_sp]).start()

    loop(sp_count, complete)

    def to_dp(i):
        e, s = i // own, lax.rem(i, own)
        return remote(
            home.at[i], out_ref.at[s, my_dp], send_4.at[i], recv_4.at[s, my_dp], my_sp, e
        )

    def is_mine(i):
        return i // own == my_dp

    def send_home(i):
        arrived(home.at[i], recv_3.at[i])

        @pl.when(jnp.logical_not(is_mine(i)))
        def _():
            to_dp(i).start()

        @pl.when(is_mine(i))
        def _():
            s = lax.rem(i, own)
            pltpu.make_async_copy(home.at[i], out_ref.at[s, my_dp], recv_4.at[s, my_dp]).start()

    loop(sp_count, send_home)
    for s in range(own):
        for q in range(dp_count):
            arrived(out_ref.at[s, q], recv_4.at[s, q])

    for step in range(1, dp_count):
        over_dp(step).wait_send()

    def finish(j):
        for x in range(pairs):
            inside(j, x).wait_send()
            chip_copy(j, x).wait_send()
        for hop in range(1, pairs):
            across(j, hop).wait_send()
            sum_copy(j, hop).wait_send()

        @pl.when(j != my_sp)
        def _():
            over_sp(j // own, lax.rem(j, own)).wait_send()
            to_sp(j).wait_send()

        @pl.when(jnp.logical_not(is_mine(j)))
        def _():
            to_dp(j).wait_send()

    loop(sp_count, finish)


def attend(block, bias, query_data, key_data, value_data, o_ref, columns):
    length = query_data.shape[0]
    log2e = math.log2(math.e)
    bias = bias * log2e
    scale = HEAD_DIM ** (-0.5) * log2e
    row = lax.broadcasted_iota(jnp.int32, (2 * block, 2 * block), 0)
    col = lax.broadcasted_iota(jnp.int32, (2 * block, 2 * block), 1)
    row = jnp.where(row >= block, row - block, row)
    summing = jnp.where(jnp.logical_or(col >= block, row > col), 1.0, 0.0).astype(jnp.bfloat16)
    at_row = lax.broadcasted_iota(jnp.int32, (block, block), 0)
    at_col = lax.broadcasted_iota(jnp.int32, (block, block), 1)
    causal = at_col < at_row
    for r in range(length // block):
        rows = slice(r * block, (r + 1) * block)
        query = query_data[rows]
        carried = None
        total = None
        for c in range(r, -1, -1):
            keys = slice(c * block, (c + 1) * block)
            scores = (
                lax.dot_general(
                    query,
                    key_data[keys],
                    (((1,), (1,)), ((), ())),
                    preferred_element_type=jnp.float32,
                )
                * scale
                + bias
            )
            soft = jnp.log2(1.0 + jnp.exp2(-jnp.abs(scores)))
            log_keep = -jnp.maximum(scores, 0.0) - soft
            log_break = jnp.minimum(scores, 0.0) - soft
            if c == r:
                log_keep = jnp.where(causal, log_keep, 0.0)
            high = log_keep.astype(jnp.bfloat16)
            low = (log_keep - high.astype(jnp.float32)).astype(jnp.bfloat16)
            sums = jnp.dot(
                jnp.concatenate((high, low), axis=1), summing, preferred_element_type=jnp.float32
            )
            exponent = log_break + sums[:, :block]
            if carried is not None:
                exponent = exponent + carried
            weights = jnp.exp2(exponent)
            if c == r:
                weights = jnp.where(causal, weights, 0.0)
            term = jnp.dot(
                weights.astype(jnp.bfloat16), value_data[keys], preferred_element_type=jnp.float32
            )
            carried = sums[:, block:] if carried is None else carried + sums[:, block:]
            total = term if total is None else total + term
        o_ref[rows, columns] = total.astype(jnp.bfloat16)


def gathered(tokens, norm_gain, w_query, w_key, w_value, break_bias, w_out):
    own, tok_rows, width = tokens.shape
    sp_count, dp_count = lax.axis_size("sp"), lax.axis_size("dp")
    part = tok_rows // dp_count
    pairs = dp_count // 2
    length = sp_count * tok_rows
    copies = w_query.shape[1] // w_key.shape[1]
    vmem = pl.BlockSpec(memory_space=pltpu.VMEM)
    hbm = pl.BlockSpec(memory_space=pl.ANY)

    def room(*shape):
        return pltpu.VMEM(shape, jnp.bfloat16)

    dma = pltpu.SemaphoreType.DMA
    mixed = pl.pallas_call(
        functools.partial(layer_kernel, sp_count, dp_count, copies, math.gcd(length, 128)),
        out_shape=jax.ShapeDtypeStruct((own, dp_count, part, width), jnp.bfloat16),
        in_specs=[vmem, vmem, pl.BlockSpec(memory_space=pltpu.SMEM), hbm, hbm, hbm, hbm],
        out_specs=vmem,
        scratch_shapes=[
            room(*w_query.shape),
            room(*w_key.shape),
            room(*w_value.shape),
            room(*w_out.shape),
            room(dp_count, own, part, width),
            room(dp_count, own, part, width),
            room(sp_count, dp_count, part, width),
            room(length, w_query.shape[1]),
            room(length, w_key.shape[1]),
            room(length, w_value.shape[1]),
            room(length, w_query.shape[1]),
            room(sp_count, dp_count, part, width),
            room(pairs, sp_count, part, width),
            room(pairs - 1, sp_count, part, width),
            room(pairs - 1, sp_count, part, width),
            room(sp_count, part, width),
            room(sp_count, part, width),
            dma((4,)),
            dma((dp_count,)),
            dma((dp_count,)),
            dma((sp_count,)),
            dma((sp_count,)),
            dma((pairs - 1, sp_count)),
            dma((pairs - 1, sp_count)),
            dma((pairs, sp_count)),
            dma((pairs, sp_count)),
            dma((pairs, sp_count)),
            dma((pairs, sp_count)),
            dma((pairs - 1, sp_count)),
            dma((pairs - 1, sp_count)),
            dma((sp_count,)),
            dma((sp_count,)),
            dma((sp_count,)),
            dma((own, dp_count)),
        ],
        compiler_params=pltpu.CompilerParams(collective_id=1, has_side_effects=True),
        name="layer",
    )(
        tokens.reshape(own, dp_count, part, width),
        norm_gain.reshape(1, width),
        break_bias,
        w_query,
        w_key,
        w_value,
        w_out,
    )
    return mixed.reshape(own, tok_rows, width)


def local(tokens, *rest):
    sp_count, dp_count = lax.axis_size("sp"), lax.axis_size("dp")
    one_each = dp_count * tokens.shape[0] == sp_count
    if one_each and dp_count % 2 == 0 and dp_count > 2 and tokens.shape[1] % (16 * dp_count) == 0:
        return gathered(tokens, *rest)
    return exchanged(tokens, *rest)


def solution(mesh):
    return jax.shard_map(
        local,
        mesh=mesh,
        in_specs=(
            P("dp", "sp", None),
            P(),
            P(None, "dp"),
            P(None, "dp"),
            P(None, "dp"),
            P("dp"),
            P("dp", None),
        ),
        out_specs=P("dp", "sp", None),
        check_vma=False,
    )
```

```python
import functools
import math

import jax
import jax.numpy as jnp
from jax import lax
from jax.experimental import pallas as pl
from jax.experimental.pallas import tpu as pltpu
from jax.sharding import PartitionSpec as P

HEAD_DIM = 128


EPS = 1e-06


def normalize(tokens):
    widened = tokens.astype(jnp.float32)
    return widened * lax.rsqrt(jnp.mean(widened * widened, axis=-1, keepdims=True) + EPS)


def head_major(normed, weight, copies):
    model_width = weight.shape[0]
    head_count = weight.shape[1] // HEAD_DIM
    result = jnp.einsum(
        "ntd,dhc->nhtc",
        normed,
        weight.reshape(model_width, head_count, HEAD_DIM),
        preferred_element_type=jnp.float32,
    ).astype(jnp.bfloat16)
    return jnp.repeat(result, copies, axis=1)


def stick_item(operands):
    query_data, key_data, value_data, bias_term = operands
    seq_length = query_data.shape[0]
    block_size = math.gcd(seq_length, 512)
    head_scale = HEAD_DIM ** (-0.5)
    offsets = jnp.arange(block_size, dtype=jnp.int32)

    def query_block(block_index):
        query_rows = lax.dynamic_slice_in_dim(query_data, block_index * block_size, block_size, 0)
        query_pos = block_index * block_size + offsets

        def key_block(step_count, carry):
            carried, accumulated = carry
            key_index = block_index - step_count
            key_rows = lax.dynamic_slice_in_dim(key_data, key_index * block_size, block_size, 0)
            value_rows = lax.dynamic_slice_in_dim(value_data, key_index * block_size, block_size, 0)
            key_pos = key_index * block_size + offsets
            scores = (
                jnp.einsum("qc,kc->qk", query_rows, key_rows, preferred_element_type=jnp.float32)
                * head_scale
                + bias_term
            )
            causal = key_pos[None, :] < query_pos[:, None]
            log_keep = jnp.where(causal, jax.nn.log_sigmoid(-scores), 0.0)
            after_sum = lax.cumsum(log_keep, axis=1, reverse=True) - log_keep + carried[:, None]
            weights = jnp.where(
                causal, jnp.exp(jax.nn.log_sigmoid(scores) + after_sum), 0.0
            ).astype(jnp.bfloat16)
            accumulated = accumulated + jnp.dot(
                weights, value_rows, preferred_element_type=jnp.float32
            )
            return (carried + jnp.sum(log_keep, axis=1), accumulated)

        initial = (
            jnp.zeros((block_size,), jnp.float32),
            jnp.zeros((block_size, HEAD_DIM), jnp.float32),
        )
        carried, accumulated = lax.fori_loop(0, block_index + 1, key_block, initial)
        return accumulated.astype(jnp.bfloat16)

    blocks = lax.map(query_block, jnp.arange(seq_length // block_size, dtype=jnp.int32))
    return blocks.reshape(seq_length, HEAD_DIM)


def exchanged(tokens, norm_gain, w_query, w_key, w_value, break_bias, w_out):
    own_seqs = tokens.shape[0]
    seq_count = lax.axis_size("dp") * own_seqs
    seq_parts = lax.axis_size("sp")
    local_heads = w_query.shape[1] // HEAD_DIM
    copies = local_heads // (w_key.shape[1] // HEAD_DIM)
    tok_rows = tokens.shape[1]
    model_width = tokens.shape[2]
    item_count = seq_count * local_heads
    normed = (normalize(lax.all_gather(tokens, "dp", axis=0, tiled=True)) * norm_gain).astype(
        jnp.bfloat16
    )
    combined = jnp.concatenate(
        (
            head_major(normed, w_query, 1),
            head_major(normed, w_key, copies),
            head_major(normed, w_value, copies),
        ),
        axis=3,
    )
    arrived = lax.all_to_all(
        combined.reshape(item_count, tok_rows, 3 * HEAD_DIM),
        "sp",
        split_axis=0,
        concat_axis=1,
        tiled=True,
    )
    query_data = arrived[:, :, :HEAD_DIM]
    key_data = arrived[:, :, HEAD_DIM : 2 * HEAD_DIM]
    value_data = arrived[:, :, 2 * HEAD_DIM :]
    per_device = item_count // seq_parts
    item_ids = lax.axis_index("sp") * per_device + jnp.arange(per_device, dtype=jnp.int32)
    local_ids = item_ids % local_heads
    bias_items = jnp.sum(
        jnp.where(
            local_ids[:, None] == jnp.arange(local_heads, dtype=jnp.int32)[None, :],
            break_bias[None, :],
            0.0,
        ),
        axis=1,
    )
    attended = lax.map(stick_item, (query_data, key_data, value_data, bias_items))
    returned = lax.all_to_all(attended, "sp", split_axis=1, concat_axis=0, tiled=True)
    grouped = returned.reshape(seq_count, local_heads, tok_rows, HEAD_DIM)
    out_weight = w_out.reshape(local_heads, HEAD_DIM, model_width)
    term_rows = jnp.einsum(
        "nhtc,hcd->ntd", grouped, out_weight, preferred_element_type=jnp.float32
    ).astype(jnp.bfloat16)
    term_rows = lax.optimization_barrier(term_rows)
    summed = lax.psum_scatter(
        term_rows.astype(jnp.float32).astype(jnp.bfloat16), "dp", scatter_dimension=0, tiled=True
    ).astype(jnp.float32)
    return normalize(summed).astype(jnp.bfloat16)


def remote(src, dst, send_sem, recv_sem, sp, dp):
    return pltpu.make_async_remote_copy(
        src_ref=src,
        dst_ref=dst,
        send_sem=send_sem,
        recv_sem=recv_sem,
        device_id={"sp": sp, "dp": dp},
        device_id_type=pl.DeviceIdType.MESH,
    )


def greet(sp, dp):
    pl.semaphore_signal(
        pltpu.get_barrier_semaphore(),
        inc=1,
        device_id={"sp": sp, "dp": dp},
        device_id_type=pl.DeviceIdType.MESH,
    )


def loop(count, body):
    lax.fori_loop(0, count, lambda step, carry: (body(step), carry)[1], 0)


def layer_kernel(
    sp_count, dp_count, copies, block, x_ref, gain_ref, bias_ref, wq_hbm, wk_hbm, wv_hbm, wo_hbm, out_ref,
    wq, wk, wv, wo, normed, staged, rows_ref, q_ref, k_ref, v_ref, att_ref, p_ref, from_core, summed,
    from_x, done, home, load_sem, send_1, recv_1, send_2, recv_2, send_x, recv_x, send_p, recv_p,
    send_c, recv_c, send_s, recv_s, send_3, recv_3, send_4, recv_4,
):
    my_sp, my_dp = lax.axis_index("sp"), lax.axis_index("dp")
    own, _, part, width = x_ref.shape
    pairs = dp_count // 2
    my_x, my_core = my_dp // 2, lax.rem(my_dp, 2)
    other = my_x * 2 + 1 - my_core
    length = sp_count * dp_count * part

    def at_hop(hop):
        return lax.rem(my_x + hop, pairs)

    def peer(step):
        hop, flip = step // 2, step % 2
        return at_hop(hop) * 2 + (1 - my_core if flip else my_core)

    loop(sp_count - 1, lambda step: greet(lax.rem(my_sp + step + 1, sp_count), my_dp))
    for step in range(1, dp_count):
        greet(my_sp, lax.rem(my_dp + step, dp_count))

    loads = [
        pltpu.make_async_copy(source, target, load_sem.at[place])
        for place, (source, target) in enumerate(
            ((wq_hbm, wq), (wk_hbm, wk), (wv_hbm, wv), (wo_hbm, wo))
        )
    ]
    for load in loads:
        load.start()

    for s in range(own):
        for q in range(dp_count):
            normed[q, s] = (normalize(x_ref[s, q]) * gain_ref[...]).astype(jnp.bfloat16)
    staged[my_dp] = normed[my_dp]
    pl.semaphore_wait(pltpu.get_barrier_semaphore(), sp_count + dp_count - 2)

    def over_dp(step):
        q = peer(step)
        return remote(
            normed.at[q], staged.at[my_dp], send_1.at[step], recv_1.at[my_dp], my_sp, q
        )

    def arrived(ref, sem):
        pltpu.make_async_copy(ref, ref, sem).wait()

    order = list(range(2, dp_count)) + [1]
    for step in order:
        over_dp(step).start()

    def over_sp(e, s):
        i = e * own + s
        return remote(
            staged.at[e, s], rows_ref.at[my_sp, my_dp], send_2.at[i], recv_2.at[my_sp], i, my_dp
        )

    for step in [0, 1] + list(range(2, dp_count)):
        e = peer(step)
        if step:
            arrived(staged.at[e], recv_1.at[e])
        for s in range(own):

            @pl.when(e * own + s != my_sp)
            def _():
                over_sp(e, s).start()

            @pl.when(e * own + s == my_sp)
            def _():
                pltpu.make_async_copy(
                    staged.at[e, s], rows_ref.at[my_sp, my_dp], recv_2.at[my_sp]
                ).start()

    def across(j, hop):
        piece = rows_ref.at[j, my_dp]
        return remote(
            piece, piece, send_x.at[hop - 1, j], recv_x.at[hop - 1, j], my_sp, at_hop(hop) * 2 + my_core
        )

    def inside(j, x):
        piece = rows_ref.at[j, x * 2 + my_core]
        return remote(piece, piece, send_p.at[x, j], recv_p.at[x, j], my_sp, other)

    def hand_on(step):
        j = lax.rem(my_sp + step, sp_count)
        arrived(rows_ref.at[j, my_dp], recv_2.at[j])
        for hop in range(1, pairs):
            across(j, hop).start()
        inside(j, my_x).start()

    loop(sp_count, hand_on)

    def relay(step):
        j = lax.rem(my_sp + step, sp_count)
        for hop in range(1, pairs):
            x = at_hop(pairs - hop)
            arrived(rows_ref.at[j, x * 2 + my_core], recv_x.at[hop - 1, j])
            inside(j, x).start()

    def finish_rows(hop):
        x = at_hop(hop)
        loop(
            sp_count,
            lambda j: arrived(rows_ref.at[j, x * 2 + 1 - my_core], recv_p.at[x, j]),
        )

    tiles = []
    for weight, target in ((wk, k_ref), (wv, v_ref), (wq, q_ref)):
        columns = math.gcd(weight.shape[1], 256)
        for start in range(0, weight.shape[1], columns):
            tiles.append((weight, target, slice(start, start + columns)))

    def project(hop, tile):
        weight, target, at = tile
        chip = pl.ds(at_hop(hop) * 2, 2)
        value = jnp.dot(
            rows_ref[:, chip].reshape(length // pairs, width),
            weight[:, at],
            preferred_element_type=jnp.float32,
        ).astype(jnp.bfloat16)
        target[:, chip, :, at] = value.reshape(sp_count, 2, part, value.shape[1])

    finish_rows(0)
    for load in loads[:3]:
        load.wait()
    for step in range(max(sp_count, len(tiles))):
        if step < len(tiles):
            project(0, tiles[step])
        if step < sp_count:
            relay(step)
    for hop in range(1, pairs):
        finish_rows(hop)
        for tile in tiles:
            project(hop, tile)
    loads[3].wait()

    def head(h):
        mine = pl.ds(pl.multiple_of(h * HEAD_DIM, HEAD_DIM), HEAD_DIM)
        shared = pl.ds(pl.multiple_of(h // copies * HEAD_DIM, HEAD_DIM), HEAD_DIM)
        query_data, key_data, value_data = (
            ref[:, :, :, at].reshape(length, HEAD_DIM)
            for ref, at in ((q_ref, mine), (k_ref, shared), (v_ref, shared))
        )
        attend(block, bias_ref[h], query_data, key_data, value_data, att_ref, mine)

    loop(q_ref.shape[3] // HEAD_DIM, head)

    def chip_copy(j, hop):
        return remote(
            p_ref.at[j, at_hop(hop) * 2 + 1 - my_core],
            from_core.at[hop, j],
            send_c.at[hop, j],
            recv_c.at[hop, j],
            my_sp,
            other,
        )

    def sum_copy(j, hop):
        return remote(
            summed.at[hop - 1, j],
            from_x.at[hop - 1, j],
            send_s.at[hop - 1, j],
            recv_s.at[hop - 1, j],
            my_sp,
            at_hop(hop) * 2 + my_core,
        )

    hops = list(range(1, pairs)) + [0]
    some = math.gcd(sp_count, 2)
    group = sp_count // some
    wide = math.gcd(width, 512)
    tall = group * dp_count * part

    def send_sums(j):
        for hop in range(1, pairs):
            chip_copy(j, hop).wait_recv()
            mine = p_ref[j, at_hop(hop) * 2 + my_core].astype(jnp.float32)
            summed[hop - 1, j] = (mine + from_core[hop, j].astype(jnp.float32)).astype(jnp.bfloat16)
            sum_copy(j, hop).start()

    for r in range(some):
        heads = att_ref[r * tall : (r + 1) * tall, :]

        def out_tile(n):
            at = pl.ds(pl.multiple_of(n * wide, wide), wide)
            value = jnp.dot(heads, wo[:, at], preferred_element_type=jnp.float32)
            p_ref[r * group : (r + 1) * group, :, :, at] = value.astype(jnp.bfloat16).reshape(
                group, dp_count, part, wide
            )

        loop(width // wide, out_tile)
        for hop in hops:
            loop(group, lambda j: chip_copy(r * group + j, hop).start())
        loop(group, lambda j: send_sums(r * group + j))

    def to_sp(j):
        return remote(done.at[j], home.at[my_sp], send_3.at[j], recv_3.at[my_sp], j, my_dp)

    def complete(j):
        chip_copy(j, 0).wait_recv()
        total = p_ref[j, my_dp].astype(jnp.float32) + from_core[0, j].astype(jnp.float32)
        for hop in range(1, pairs):
            sum_copy(j, hop).wait_recv()
            total = total + from_x[hop - 1, j].astype(jnp.float32)
        done[j] = normalize(total).astype(jnp.bfloat16)

        @pl.when(j != my_sp)
        def _():
            to_sp(j).start()

        @pl.when(j == my_sp)
        def _():
            pltpu.make_async_copy(done.at[j], home.at[my_sp], recv_3.at[my_sp]).start()

    loop(sp_count, complete)

    def to_dp(i):
        e, s = i // own, lax.rem(i, own)
        return remote(
            home.at[i], out_ref.at[s, my_dp], send_4.at[i], recv_4.at[s, my_dp], my_sp, e
        )

    def is_mine(i):
        return i // own == my_dp

    def send_home(i):
        arrived(home.at[i], recv_3.at[i])

        @pl.when(jnp.logical_not(is_mine(i)))
        def _():
            to_dp(i).start()

        @pl.when(is_mine(i))
        def _():
            s = lax.rem(i, own)
            pltpu.make_async_copy(home.at[i], out_ref.at[s, my_dp], recv_4.at[s, my_dp]).start()

    loop(sp_count, send_home)
    for s in range(own):
        for q in range(dp_count):
            arrived(out_ref.at[s, q], recv_4.at[s, q])

    for step in range(1, dp_count):
        over_dp(step).wait_send()

    def finish(j):
        for x in range(pairs):
            inside(j, x).wait_send()
            chip_copy(j, x).wait_send()
        for hop in range(1, pairs):
            across(j, hop).wait_send()
            sum_copy(j, hop).wait_send()

        @pl.when(j != my_sp)
        def _():
            over_sp(j // own, lax.rem(j, own)).wait_send()
            to_sp(j).wait_send()

        @pl.when(jnp.logical_not(is_mine(j)))
        def _():
            to_dp(j).wait_send()

    loop(sp_count, finish)


def below(first, rest):
    return jnp.concatenate((first, rest), axis=0) if rest.shape[0] else first


def attend(block, bias, query_data, key_data, value_data, o_ref, columns):
    length = query_data.shape[0]
    log2e = math.log2(math.e)
    bias = bias * log2e
    scale = HEAD_DIM ** (-0.5) * log2e
    row = lax.broadcasted_iota(jnp.int32, (2 * block, 2 * block), 0)
    col = lax.broadcasted_iota(jnp.int32, (2 * block, 2 * block), 1)
    row = jnp.where(row >= block, row - block, row)
    summing = jnp.where(jnp.logical_or(col >= block, row > col), 1.0, 0.0).astype(jnp.bfloat16)
    at_row = lax.broadcasted_iota(jnp.int32, (block, block), 0)
    at_col = lax.broadcasted_iota(jnp.int32, (block, block), 1)
    causal = at_col < at_row
    carried = None
    total = None
    for c in range(length // block - 1, -1, -1):
        keys = slice(c * block, (c + 1) * block)
        scores = (
            lax.dot_general(
                query_data[c * block :],
                key_data[keys],
                (((1,), (1,)), ((), ())),
                preferred_element_type=jnp.float32,
            )
            * scale
            + bias
        )
        soft = jnp.log2(1.0 + jnp.exp2(-jnp.abs(scores)))
        log_keep = -jnp.maximum(scores, 0.0) - soft
        log_break = jnp.minimum(scores, 0.0) - soft
        log_keep = below(jnp.where(causal, log_keep[:block], 0.0), log_keep[block:])
        high = log_keep.astype(jnp.bfloat16)
        low = (log_keep - high.astype(jnp.float32)).astype(jnp.bfloat16)
        sums = jnp.dot(
            jnp.concatenate((high, low), axis=1), summing, preferred_element_type=jnp.float32
        )
        exponent = log_break + sums[:, :block]
        if carried is None:
            carried = sums[:, block:]
        else:
            exponent = below(exponent[:block], exponent[block:] + carried)
            carried = below(sums[:block, block:], sums[block:, block:] + carried)
        weights = jnp.exp2(exponent)
        weights = below(jnp.where(causal, weights[:block], 0.0), weights[block:])
        term = jnp.dot(
            weights.astype(jnp.bfloat16), value_data[keys], preferred_element_type=jnp.float32
        )
        total = term if total is None else below(term[:block], term[block:] + total)
    o_ref[:, columns] = total.astype(jnp.bfloat16)


def gathered(tokens, norm_gain, w_query, w_key, w_value, break_bias, w_out):
    own, tok_rows, width = tokens.shape
    sp_count, dp_count = lax.axis_size("sp"), lax.axis_size("dp")
    part = tok_rows // dp_count
    pairs = dp_count // 2
    length = sp_count * tok_rows
    copies = w_query.shape[1] // w_key.shape[1]
    vmem = pl.BlockSpec(memory_space=pltpu.VMEM)
    hbm = pl.BlockSpec(memory_space=pl.ANY)

    def room(*shape):
        return pltpu.VMEM(shape, jnp.bfloat16)

    dma = pltpu.SemaphoreType.DMA
    mixed = pl.pallas_call(
        functools.partial(layer_kernel, sp_count, dp_count, copies, math.gcd(length, 128)),
        out_shape=jax.ShapeDtypeStruct((own, dp_count, part, width), jnp.bfloat16),
        in_specs=[vmem, vmem, pl.BlockSpec(memory_space=pltpu.SMEM), hbm, hbm, hbm, hbm],
        out_specs=vmem,
        scratch_shapes=[
            room(*w_query.shape),
            room(*w_key.shape),
            room(*w_value.shape),
            room(*w_out.shape),
            room(dp_count, own, part, width),
            room(dp_count, own, part, width),
            room(sp_count, dp_count, part, width),
            room(sp_count, dp_count, part, w_query.shape[1]),
            room(sp_count, dp_count, part, w_key.shape[1]),
            room(sp_count, dp_count, part, w_value.shape[1]),
            room(length, w_query.shape[1]),
            room(sp_count, dp_count, part, width),
            room(pairs, sp_count, part, width),
            room(pairs - 1, sp_count, part, width),
            room(pairs - 1, sp_count, part, width),
            room(sp_count, part, width),
            room(sp_count, part, width),
            dma((4,)),
            dma((dp_count,)),
            dma((dp_count,)),
            dma((sp_count,)),
            dma((sp_count,)),
            dma((pairs - 1, sp_count)),
            dma((pairs - 1, sp_count)),
            dma((pairs, sp_count)),
            dma((pairs, sp_count)),
            dma((pairs, sp_count)),
            dma((pairs, sp_count)),
            dma((pairs - 1, sp_count)),
            dma((pairs - 1, sp_count)),
            dma((sp_count,)),
            dma((sp_count,)),
            dma((sp_count,)),
            dma((own, dp_count)),
        ],
        compiler_params=pltpu.CompilerParams(collective_id=1, has_side_effects=True),
        name="layer",
    )(
        tokens.reshape(own, dp_count, part, width),
        norm_gain.reshape(1, width),
        break_bias,
        w_query,
        w_key,
        w_value,
        w_out,
    )
    return mixed.reshape(own, tok_rows, width)


def local(tokens, *rest):
    sp_count, dp_count = lax.axis_size("sp"), lax.axis_size("dp")
    one_each = dp_count * tokens.shape[0] == sp_count
    if one_each and dp_count % 2 == 0 and dp_count > 2 and tokens.shape[1] % (16 * dp_count) == 0:
        return gathered(tokens, *rest)
    return exchanged(tokens, *rest)


def solution(mesh):
    return jax.shard_map(
        local,
        mesh=mesh,
        in_specs=(
            P("dp", "sp", None),
            P(),
            P(None, "dp"),
            P(None, "dp"),
            P(None, "dp"),
            P("dp"),
            P("dp", None),
        ),
        out_specs=P("dp", "sp", None),
        check_vma=False,
    )
```

```python
import functools
import math

import jax
import jax.numpy as jnp
from jax import lax
from jax.experimental import pallas as pl
from jax.experimental.pallas import tpu as pltpu
from jax.sharding import PartitionSpec as P

HEAD_DIM = 128


EPS = 1e-06


def normalize(tokens):
    widened = tokens.astype(jnp.float32)
    return widened * lax.rsqrt(jnp.mean(widened * widened, axis=-1, keepdims=True) + EPS)


def head_major(normed, weight, copies):
    model_width = weight.shape[0]
    head_count = weight.shape[1] // HEAD_DIM
    result = jnp.einsum(
        "ntd,dhc->nhtc",
        normed,
        weight.reshape(model_width, head_count, HEAD_DIM),
        preferred_element_type=jnp.float32,
    ).astype(jnp.bfloat16)
    return jnp.repeat(result, copies, axis=1)


def stick_item(operands):
    query_data, key_data, value_data, bias_term = operands
    seq_length = query_data.shape[0]
    block_size = math.gcd(seq_length, 512)
    head_scale = HEAD_DIM ** (-0.5)
    offsets = jnp.arange(block_size, dtype=jnp.int32)

    def query_block(block_index):
        query_rows = lax.dynamic_slice_in_dim(query_data, block_index * block_size, block_size, 0)
        query_pos = block_index * block_size + offsets

        def key_block(step_count, carry):
            carried, accumulated = carry
            key_index = block_index - step_count
            key_rows = lax.dynamic_slice_in_dim(key_data, key_index * block_size, block_size, 0)
            value_rows = lax.dynamic_slice_in_dim(value_data, key_index * block_size, block_size, 0)
            key_pos = key_index * block_size + offsets
            scores = (
                jnp.einsum("qc,kc->qk", query_rows, key_rows, preferred_element_type=jnp.float32)
                * head_scale
                + bias_term
            )
            causal = key_pos[None, :] < query_pos[:, None]
            log_keep = jnp.where(causal, jax.nn.log_sigmoid(-scores), 0.0)
            after_sum = lax.cumsum(log_keep, axis=1, reverse=True) - log_keep + carried[:, None]
            weights = jnp.where(
                causal, jnp.exp(jax.nn.log_sigmoid(scores) + after_sum), 0.0
            ).astype(jnp.bfloat16)
            accumulated = accumulated + jnp.dot(
                weights, value_rows, preferred_element_type=jnp.float32
            )
            return (carried + jnp.sum(log_keep, axis=1), accumulated)

        initial = (
            jnp.zeros((block_size,), jnp.float32),
            jnp.zeros((block_size, HEAD_DIM), jnp.float32),
        )
        carried, accumulated = lax.fori_loop(0, block_index + 1, key_block, initial)
        return accumulated.astype(jnp.bfloat16)

    blocks = lax.map(query_block, jnp.arange(seq_length // block_size, dtype=jnp.int32))
    return blocks.reshape(seq_length, HEAD_DIM)


def exchanged(tokens, norm_gain, w_query, w_key, w_value, break_bias, w_out):
    own_seqs = tokens.shape[0]
    seq_count = lax.axis_size("dp") * own_seqs
    seq_parts = lax.axis_size("sp")
    local_heads = w_query.shape[1] // HEAD_DIM
    copies = local_heads // (w_key.shape[1] // HEAD_DIM)
    tok_rows = tokens.shape[1]
    model_width = tokens.shape[2]
    item_count = seq_count * local_heads
    normed = (normalize(lax.all_gather(tokens, "dp", axis=0, tiled=True)) * norm_gain).astype(
        jnp.bfloat16
    )
    combined = jnp.concatenate(
        (
            head_major(normed, w_query, 1),
            head_major(normed, w_key, copies),
            head_major(normed, w_value, copies),
        ),
        axis=3,
    )
    arrived = lax.all_to_all(
        combined.reshape(item_count, tok_rows, 3 * HEAD_DIM),
        "sp",
        split_axis=0,
        concat_axis=1,
        tiled=True,
    )
    query_data = arrived[:, :, :HEAD_DIM]
    key_data = arrived[:, :, HEAD_DIM : 2 * HEAD_DIM]
    value_data = arrived[:, :, 2 * HEAD_DIM :]
    per_device = item_count // seq_parts
    item_ids = lax.axis_index("sp") * per_device + jnp.arange(per_device, dtype=jnp.int32)
    local_ids = item_ids % local_heads
    bias_items = jnp.sum(
        jnp.where(
            local_ids[:, None] == jnp.arange(local_heads, dtype=jnp.int32)[None, :],
            break_bias[None, :],
            0.0,
        ),
        axis=1,
    )
    attended = lax.map(stick_item, (query_data, key_data, value_data, bias_items))
    returned = lax.all_to_all(attended, "sp", split_axis=1, concat_axis=0, tiled=True)
    grouped = returned.reshape(seq_count, local_heads, tok_rows, HEAD_DIM)
    out_weight = w_out.reshape(local_heads, HEAD_DIM, model_width)
    term_rows = jnp.einsum(
        "nhtc,hcd->ntd", grouped, out_weight, preferred_element_type=jnp.float32
    ).astype(jnp.bfloat16)
    term_rows = lax.optimization_barrier(term_rows)
    summed = lax.psum_scatter(
        term_rows.astype(jnp.float32).astype(jnp.bfloat16), "dp", scatter_dimension=0, tiled=True
    ).astype(jnp.float32)
    return normalize(summed).astype(jnp.bfloat16)


def remote(src, dst, send_sem, recv_sem, sp, dp):
    return pltpu.make_async_remote_copy(
        src_ref=src,
        dst_ref=dst,
        send_sem=send_sem,
        recv_sem=recv_sem,
        device_id={"sp": sp, "dp": dp},
        device_id_type=pl.DeviceIdType.MESH,
    )


def greet(sp, dp):
    pl.semaphore_signal(
        pltpu.get_barrier_semaphore(),
        inc=1,
        device_id={"sp": sp, "dp": dp},
        device_id_type=pl.DeviceIdType.MESH,
    )


def loop(count, body):
    lax.fori_loop(0, count, lambda step, carry: (body(step), carry)[1], 0)


def layer_kernel(
    sp_count, dp_count, copies, block, x_ref, gain_ref, bias_ref, wq_hbm, wk_hbm, wv_hbm, wo_hbm, out_ref,
    wq, wk, wv, wo, normed, staged, rows_ref, q_ref, k_ref, v_ref, att_ref, p_ref, from_core, summed,
    from_x, done, home, load_sem, send_1, recv_1, send_2, recv_2, send_x, recv_x, send_p, recv_p,
    send_c, recv_c, send_s, recv_s, send_3, recv_3, send_4, recv_4,
):
    my_sp, my_dp = lax.axis_index("sp"), lax.axis_index("dp")
    own, _, part, width = x_ref.shape
    pairs = dp_count // 2
    my_x, my_core = my_dp // 2, lax.rem(my_dp, 2)
    other = my_x * 2 + 1 - my_core
    length = sp_count * dp_count * part

    def at_hop(hop):
        return lax.rem(my_x + hop, pairs)

    def peer(step):
        hop, flip = step // 2, step % 2
        return at_hop(hop) * 2 + (1 - my_core if flip else my_core)

    loop(sp_count - 1, lambda step: greet(lax.rem(my_sp + step + 1, sp_count), my_dp))
    for step in range(1, dp_count):
        greet(my_sp, lax.rem(my_dp + step, dp_count))

    loads = [
        pltpu.make_async_copy(source, target, load_sem.at[place])
        for place, (source, target) in enumerate(
            ((wq_hbm, wq), (wk_hbm, wk), (wv_hbm, wv), (wo_hbm, wo))
        )
    ]
    for load in loads:
        load.start()

    for s in range(own):
        for q in range(dp_count):
            normed[q, s] = (normalize(x_ref[s, q]) * gain_ref[...]).astype(jnp.bfloat16)
    staged[my_dp] = normed[my_dp]
    pl.semaphore_wait(pltpu.get_barrier_semaphore(), sp_count + dp_count - 2)

    def over_dp(step):
        q = peer(step)
        return remote(
            normed.at[q], staged.at[my_dp], send_1.at[step], recv_1.at[my_dp], my_sp, q
        )

    def arrived(ref, sem):
        pltpu.make_async_copy(ref, ref, sem).wait()

    order = list(range(2, dp_count)) + [1]
    for step in order:
        over_dp(step).start()

    def over_sp(e, s):
        i = e * own + s
        return remote(
            staged.at[e, s], rows_ref.at[my_sp, my_dp], send_2.at[i], recv_2.at[my_sp], i, my_dp
        )

    for step in [0, 1] + list(range(2, dp_count)):
        e = peer(step)
        if step:
            arrived(staged.at[e], recv_1.at[e])
        for s in range(own):

            @pl.when(e * own + s != my_sp)
            def _():
                over_sp(e, s).start()

            @pl.when(e * own + s == my_sp)
            def _():
                pltpu.make_async_copy(
                    staged.at[e, s], rows_ref.at[my_sp, my_dp], recv_2.at[my_sp]
                ).start()

    def across(j, hop):
        piece = rows_ref.at[j, my_dp]
        return remote(
            piece, piece, send_x.at[hop - 1, j], recv_x.at[hop - 1, j], my_sp, at_hop(hop) * 2 + my_core
        )

    def inside(j, x):
        piece = rows_ref.at[j, x * 2 + my_core]
        return remote(piece, piece, send_p.at[x, j], recv_p.at[x, j], my_sp, other)

    def hand_on(step):
        j = lax.rem(my_sp + step, sp_count)
        arrived(rows_ref.at[j, my_dp], recv_2.at[j])
        for hop in range(1, pairs):
            across(j, hop).start()
        inside(j, my_x).start()

    loop(sp_count, hand_on)

    def relay(step):
        j = lax.rem(my_sp + step, sp_count)
        for hop in range(1, pairs):
            x = at_hop(pairs - hop)
            arrived(rows_ref.at[j, x * 2 + my_core], recv_x.at[hop - 1, j])
            inside(j, x).start()

    def finish_rows(hop):
        x = at_hop(hop)
        loop(
            sp_count,
            lambda j: arrived(rows_ref.at[j, x * 2 + 1 - my_core], recv_p.at[x, j]),
        )

    tiles = []
    for weight, target in ((wk, k_ref), (wv, v_ref), (wq, q_ref)):
        columns = math.gcd(weight.shape[1], 256)
        for start in range(0, weight.shape[1], columns):
            tiles.append((weight, target, slice(start, start + columns)))

    def project(hop, tile):
        weight, target, at = tile
        chip = pl.ds(at_hop(hop) * 2, 2)
        value = jnp.dot(
            rows_ref[:, chip].reshape(length // pairs, width),
            weight[:, at],
            preferred_element_type=jnp.float32,
        ).astype(jnp.bfloat16)
        target[:, chip, :, at] = value.reshape(sp_count, 2, part, value.shape[1])

    finish_rows(0)
    for load in loads[:3]:
        load.wait()
    for step in range(max(sp_count, len(tiles))):
        if step < len(tiles):
            project(0, tiles[step])
        if step < sp_count:
            relay(step)
    for hop in range(1, pairs):
        finish_rows(hop)
        for tile in tiles:
            project(hop, tile)
    loads[3].wait()

    def head(h):
        mine = pl.ds(pl.multiple_of(h * HEAD_DIM, HEAD_DIM), HEAD_DIM)
        shared = pl.ds(pl.multiple_of(h // copies * HEAD_DIM, HEAD_DIM), HEAD_DIM)
        query_data, key_data, value_data = (
            ref[:, :, :, at].reshape(length, HEAD_DIM)
            for ref, at in ((q_ref, mine), (k_ref, shared), (v_ref, shared))
        )
        attend(block, bias_ref[h], query_data, key_data, value_data, att_ref, mine)

    loop(q_ref.shape[3] // HEAD_DIM, head)

    def chip_copy(j, hop):
        return remote(
            p_ref.at[j, at_hop(hop) * 2 + 1 - my_core],
            from_core.at[hop, j],
            send_c.at[hop, j],
            recv_c.at[hop, j],
            my_sp,
            other,
        )

    def sum_copy(j, hop):
        return remote(
            summed.at[hop - 1, j],
            from_x.at[hop - 1, j],
            send_s.at[hop - 1, j],
            recv_s.at[hop - 1, j],
            my_sp,
            at_hop(hop) * 2 + my_core,
        )

    hops = list(range(1, pairs)) + [0]
    wide = math.gcd(width, 512)

    def turn(step):
        return lax.rem(my_sp + step, sp_count)

    def send_sums(step):
        j = turn(step)
        for hop in range(1, pairs):
            chip_copy(j, hop).wait_recv()
            mine = p_ref[j, at_hop(hop) * 2 + my_core].astype(jnp.float32)
            summed[hop - 1, j] = (mine + from_core[hop, j].astype(jnp.float32)).astype(jnp.bfloat16)
            sum_copy(j, hop).start()

    for hop in hops:
        chip = pl.ds(at_hop(hop) * 2, 2)
        heads = att_ref[:, chip].reshape(length // pairs, att_ref.shape[3])

        def out_tile(n):
            at = pl.ds(pl.multiple_of(n * wide, wide), wide)
            value = jnp.dot(heads, wo[:, at], preferred_element_type=jnp.float32)
            p_ref[:, chip, :, at] = value.astype(jnp.bfloat16).reshape(sp_count, 2, part, wide)

        loop(width // wide, out_tile)
        loop(sp_count, lambda step: chip_copy(turn(step), hop).start())
        if hop == pairs - 1:
            loop(sp_count, send_sums)

    def to_sp(j):
        return remote(done.at[j], home.at[my_sp], send_3.at[j], recv_3.at[my_sp], j, my_dp)

    def complete(step):
        j = turn(step)
        chip_copy(j, 0).wait_recv()
        total = p_ref[j, my_dp].astype(jnp.float32) + from_core[0, j].astype(jnp.float32)
        for hop in range(1, pairs):
            sum_copy(j, hop).wait_recv()
            total = total + from_x[hop - 1, j].astype(jnp.float32)
        done[j] = normalize(total).astype(jnp.bfloat16)

        @pl.when(j != my_sp)
        def _():
            to_sp(j).start()

        @pl.when(j == my_sp)
        def _():
            pltpu.make_async_copy(done.at[j], home.at[my_sp], recv_3.at[my_sp]).start()


    def to_dp(i):
        e, s = i // own, lax.rem(i, own)
        return remote(
            home.at[i], out_ref.at[s, my_dp], send_4.at[i], recv_4.at[s, my_dp], my_sp, e
        )

    def is_mine(i):
        return i // own == my_dp

    def send_home(step):
        i = lax.rem(my_sp - step + sp_count, sp_count)
        arrived(home.at[i], recv_3.at[i])

        @pl.when(jnp.logical_not(is_mine(i)))
        def _():
            to_dp(i).start()

        @pl.when(is_mine(i))
        def _():
            s = lax.rem(i, own)
            pltpu.make_async_copy(home.at[i], out_ref.at[s, my_dp], recv_4.at[s, my_dp]).start()

    lag = min(2, sp_count)
    loop(lag, complete)

    def both(step):
        complete(step + lag)
        send_home(step)

    loop(sp_count - lag, both)
    loop(lag, lambda step: send_home(step + sp_count - lag))
    for s in range(own):
        for q in range(dp_count):
            arrived(out_ref.at[s, q], recv_4.at[s, q])

    for step in range(1, dp_count):
        over_dp(step).wait_send()

    def finish(j):
        for x in range(pairs):
            inside(j, x).wait_send()
            chip_copy(j, x).wait_send()
        for hop in range(1, pairs):
            across(j, hop).wait_send()
            sum_copy(j, hop).wait_send()

        @pl.when(j != my_sp)
        def _():
            over_sp(j // own, lax.rem(j, own)).wait_send()
            to_sp(j).wait_send()

        @pl.when(jnp.logical_not(is_mine(j)))
        def _():
            to_dp(j).wait_send()

    loop(sp_count, finish)


def below(first, rest):
    return jnp.concatenate((first, rest), axis=0) if rest.shape[0] else first


def attend(block, bias, query_data, key_data, value_data, o_ref, columns):
    length = query_data.shape[0]
    log2e = math.log2(math.e)
    bias = bias * log2e
    scale = HEAD_DIM ** (-0.5) * log2e
    row = lax.broadcasted_iota(jnp.int32, (2 * block, 2 * block), 0)
    col = lax.broadcasted_iota(jnp.int32, (2 * block, 2 * block), 1)
    row = jnp.where(row >= block, row - block, row)
    summing = jnp.where(jnp.logical_or(col >= block, row > col), 1.0, 0.0).astype(jnp.bfloat16)
    at_row = lax.broadcasted_iota(jnp.int32, (block, block), 0)
    at_col = lax.broadcasted_iota(jnp.int32, (block, block), 1)
    causal = at_col < at_row
    carried = None
    total = None
    for c in range(length // block - 1, -1, -1):
        keys = slice(c * block, (c + 1) * block)
        scores = (
            lax.dot_general(
                query_data[c * block :],
                key_data[keys],
                (((1,), (1,)), ((), ())),
                preferred_element_type=jnp.float32,
            )
            * scale
            + bias
        )
        soft = jnp.log2(1.0 + jnp.exp2(-jnp.abs(scores)))
        log_keep = -jnp.maximum(scores, 0.0) - soft
        log_break = jnp.minimum(scores, 0.0) - soft
        log_keep = below(jnp.where(causal, log_keep[:block], 0.0), log_keep[block:])
        high = log_keep.astype(jnp.bfloat16)
        low = (log_keep - high.astype(jnp.float32)).astype(jnp.bfloat16)
        sums = jnp.dot(
            jnp.concatenate((high, low), axis=1), summing, preferred_element_type=jnp.float32
        )
        exponent = log_break + sums[:, :block]
        if carried is None:
            carried = sums[:, block:]
        else:
            exponent = below(exponent[:block], exponent[block:] + carried)
            carried = below(sums[:block, block:], sums[block:, block:] + carried)
        weights = jnp.exp2(exponent)
        weights = below(jnp.where(causal, weights[:block], 0.0), weights[block:])
        term = jnp.dot(
            weights.astype(jnp.bfloat16), value_data[keys], preferred_element_type=jnp.float32
        )
        total = term if total is None else below(term[:block], term[block:] + total)
    o_ref[:, :, :, columns] = total.astype(jnp.bfloat16).reshape(*o_ref.shape[:3], HEAD_DIM)


def gathered(tokens, norm_gain, w_query, w_key, w_value, break_bias, w_out):
    own, tok_rows, width = tokens.shape
    sp_count, dp_count = lax.axis_size("sp"), lax.axis_size("dp")
    part = tok_rows // dp_count
    pairs = dp_count // 2
    length = sp_count * tok_rows
    copies = w_query.shape[1] // w_key.shape[1]
    vmem = pl.BlockSpec(memory_space=pltpu.VMEM)
    hbm = pl.BlockSpec(memory_space=pl.ANY)

    def room(*shape):
        return pltpu.VMEM(shape, jnp.bfloat16)

    dma = pltpu.SemaphoreType.DMA
    mixed = pl.pallas_call(
        functools.partial(layer_kernel, sp_count, dp_count, copies, math.gcd(length, 128)),
        out_shape=jax.ShapeDtypeStruct((own, dp_count, part, width), jnp.bfloat16),
        in_specs=[vmem, vmem, pl.BlockSpec(memory_space=pltpu.SMEM), hbm, hbm, hbm, hbm],
        out_specs=vmem,
        scratch_shapes=[
            room(*w_query.shape),
            room(*w_key.shape),
            room(*w_value.shape),
            room(*w_out.shape),
            room(dp_count, own, part, width),
            room(dp_count, own, part, width),
            room(sp_count, dp_count, part, width),
            room(sp_count, dp_count, part, w_query.shape[1]),
            room(sp_count, dp_count, part, w_key.shape[1]),
            room(sp_count, dp_count, part, w_value.shape[1]),
            room(sp_count, dp_count, part, w_query.shape[1]),
            room(sp_count, dp_count, part, width),
            room(pairs, sp_count, part, width),
            room(pairs - 1, sp_count, part, width),
            room(pairs - 1, sp_count, part, width),
            room(sp_count, part, width),
            room(sp_count, part, width),
            dma((4,)),
            dma((dp_count,)),
            dma((dp_count,)),
            dma((sp_count,)),
            dma((sp_count,)),
            dma((pairs - 1, sp_count)),
            dma((pairs - 1, sp_count)),
            dma((pairs, sp_count)),
            dma((pairs, sp_count)),
            dma((pairs, sp_count)),
            dma((pairs, sp_count)),
            dma((pairs - 1, sp_count)),
            dma((pairs - 1, sp_count)),
            dma((sp_count,)),
            dma((sp_count,)),
            dma((sp_count,)),
            dma((own, dp_count)),
        ],
        compiler_params=pltpu.CompilerParams(collective_id=1, has_side_effects=True),
        name="layer",
    )(
        tokens.reshape(own, dp_count, part, width),
        norm_gain.reshape(1, width),
        break_bias,
        w_query,
        w_key,
        w_value,
        w_out,
    )
    return mixed.reshape(own, tok_rows, width)


def local(tokens, *rest):
    sp_count, dp_count = lax.axis_size("sp"), lax.axis_size("dp")
    one_each = dp_count * tokens.shape[0] == sp_count
    if one_each and dp_count % 2 == 0 and dp_count > 2 and tokens.shape[1] % (16 * dp_count) == 0:
        return gathered(tokens, *rest)
    return exchanged(tokens, *rest)


def solution(mesh):
    return jax.shard_map(
        local,
        mesh=mesh,
        in_specs=(
            P("dp", "sp", None),
            P(),
            P(None, "dp"),
            P(None, "dp"),
            P(None, "dp"),
            P("dp"),
            P("dp", None),
        ),
        out_specs=P("dp", "sp", None),
        check_vma=False,
    )
```
